32 devices in a mesh: sp: 8 (over z, x), dp: 4 (over y, core).
Axes of the slice: x: 2, y: 2, z: 4, core: 2. Of those that a mesh axis runs over, the one named last changes fastest.
Arguments:
- gate_in: bfloat16 [4, 4096, 1024], P('dp', 'sp'), may hold values from -6 to 6
- value_in: bfloat16 [4, 4096, 1024], P('dp', 'sp'), may hold values from -6 to 6
- segments: int32 [4, 4096], P('dp', 'sp'), may hold values from 0 to 1, never falling along the last dimension, each value on 1 to 3072 neighbouring positions
- value_gain: bfloat16 [1024], P('sp'), may hold values from 0.099609375 to 1.8984375
- mixing: bfloat16 [8, 1024, 1024], P('sp', 'dp'), may hold values from -0.1875 to 0.1875
- mixing_bias: bfloat16 [8, 1024], P('sp'), may hold values from 0.099609375 to 1.8984375
Outputs:
- gated: bfloat16 [4, 4096, 1024], P('dp', 'sp')
The draws below stay inside these ranges and needn't reach their ends.
Inputs may be any that keep to these rules, and one draw needn't show every extreme that they name: `segments`: within each sequence the numbers never fall, every number 0 to 1 occurs, a document spans at most 3072 positions and some document spans exactly that.
All inputs are finite; a program needn't handle non-finite values.
Results may differ from the reference program's by a relative error of at most 0.0054.
Values may be sent and summed in bfloat16 or wider, within the bound.
A program may use at most 128 MiB of HBM per device.

```python
import math
import jax
import jax.numpy as jnp
import numpy as np
from jax import lax

HEAD_DIM = 128
HEADS = 8
WIDTH = 1024
BLK = 1024
TOK_DEV = 512
SEQ = 4096
SEQS = 4
DOCS = 2


def steps_of(rng, dims, pieces, low, top_value):
    loudness, own = 1.0, jax.random.fold_in(rng, 6)
    for position, parts in pieces:
        heights = jnp.exp(jax.random.uniform(jax.random.fold_in(own, position), (parts,), jnp.float32, low / len(pieces), top_value / len(pieces)))
        loudness = loudness * jnp.repeat(heights, dims[position] // parts).reshape([-1 if axis == position else 1 for axis in range(len(dims))])
    return loudness


def split_up(count, total, reach, skew):
    portions = [(1 << 20) // math.isqrt(standing ** skew) + 1 for standing in range(2, count + 1)]
    spare, given = total - reach - (count - 1), [1] * (count - 1)
    while spare > 0:
        candidates = [i for i in range(count - 1) if given[i] < reach]
        whole, remaining = sum([portions[i] for i in candidates]), spare
        for i in candidates:
            extra = min(reach - given[i], max(1, remaining * portions[i] // whole), spare)
            given[i] = given[i] + extra
            spare = spare - extra
    return np.array([reach] + given)


def uneven(stream_key, number_of, total, bound, slope):
    if number_of == 2:
        one = jax.random.randint(stream_key, (), max(1, total - bound), min(bound, total - 1) + 1)
        return jnp.stack([one, total - one])
    sizes = jnp.asarray(split_up(number_of, total, bound, slope), jnp.int32)
    twos = (number_of - 1) // 2
    source_of, sink = sizes[1:1 + 2 * twos:2], sizes[2:2 + 2 * twos:2]
    margin = jnp.minimum(source_of - 1, bound - sink)
    shifted = jax.random.randint(jax.random.fold_in(stream_key, 1), (twos,), 0, 1 << 20) % (margin + 1)
    sizes = sizes.at[1:1 + 2 * twos:2].set(source_of - shifted).at[2:2 + 2 * twos:2].set(sink + shifted)
    return sizes[jax.random.permutation(jax.random.fold_in(stream_key, 2), number_of)]


def gaussian(key, shape, scale, limit, pieces=(), held_as=jnp.bfloat16):
    gain = steps_of(key, shape, pieces, -0.22, 0.18) if pieces else 1.0
    drawn = jax.random.normal(key, shape, jnp.float32) * scale * gain
    return jnp.minimum(jnp.maximum(drawn, -limit), limit).astype(held_as)


def setup_inputs(seed: int = 0) -> dict:
    seeds = jax.random.split(jax.random.key(seed), 7)
    gate_in = gaussian(seeds[0], (SEQS, SEQ, WIDTH), 1.0, 6.0, ((0, 4), (1, 8)))
    value_in = gaussian(seeds[1], (SEQS, SEQ, WIDTH), 1.0, 6.0, ((0, 4), (1, 8)))
    segments = jax.vmap(lambda own: jnp.searchsorted(jnp.cumsum(uneven(own, DOCS, SEQ, 6 * TOK_DEV, 0)), jnp.arange(SEQ), side="right"))(jax.random.split(seeds[2], SEQS)).reshape((SEQS, SEQ)).astype(jnp.int32)
    value_gain = jnp.clip(1.0 + 0.18 * jax.random.normal(seeds[3], (WIDTH,), jnp.float32), 0.099609375, 1.8984375).astype(jnp.bfloat16)
    mixing = gaussian(seeds[4], (HEADS, BLK, BLK), BLK ** -0.5, 0.1875, ((0, 8), (1, 4)))
    mixing_bias = jnp.clip(1.0 + 0.18 * jax.random.normal(seeds[5], (HEADS, BLK), jnp.float32), 0.099609375, 1.8984375).astype(jnp.bfloat16)
    return dict(gate_in=gate_in, value_in=value_in, segments=segments, value_gain=value_gain, mixing=mixing, mixing_bias=mixing_bias)


epsilon = 1e-06

def reference(gate_in, value_in, segments, value_gain, mixing, mixing_bias):
    seqs, length, width = value_in.shape
    values = jax.nn.gelu(value_in.astype(jnp.float32)).reshape(seqs, length, HEADS, HEAD_DIM)
    scaled = values * lax.rsqrt(lax.optimization_barrier(jnp.mean(values * values, axis=-1, keepdims=True)) + epsilon)
    normed = (scaled.reshape(seqs, length, width) * value_gain.astype(jnp.float32)).astype(jnp.bfloat16)
    blocks = seqs * length // BLK
    value_blocks = normed.reshape(blocks, BLK, HEADS, HEAD_DIM)
    id_blocks = segments.reshape(blocks, BLK)
    mixing_f = mixing.astype(jnp.float32)
    bias_f = jnp.transpose(mixing_bias.astype(jnp.float32))[:, :, None]

    def one_block(pair_item):
        block_values, block_ids = pair_item
        same_doc = block_ids[:, None] == block_ids[None, :]
        masked = jnp.where(same_doc[None, :, :], mixing_f, jnp.zeros((), jnp.float32))
        summed = jnp.einsum('hts,shd->thd', masked, block_values.astype(jnp.float32))
        return (summed + bias_f).astype(jnp.bfloat16)
    mixed = lax.map(one_block, (value_blocks, id_blocks)).reshape(seqs, length, width)
    gate_f = jax.nn.gelu(gate_in.astype(jnp.float32))
    return (gate_f * mixed.astype(jnp.float32)).astype(jnp.bfloat16)
```

```python
import functools

import jax
import jax.numpy as jnp
from jax import lax
from jax.experimental import pallas as pl
from jax.experimental.pallas import tpu as pltpu
from jax.sharding import PartitionSpec as P

HEAD_DIM = 128
CORES = 2
LANES = 128
ROW_STEP = 256
PARTS = 4
MESH = pl.DeviceIdType.MESH

epsilon = 1e-06


def flip(a, b, count):
    total, bit = 0, 1
    while bit < count:
        total = total + ((a // bit + b // bit) % 2) * bit
        bit *= 2
    return total


def gelu(x):
    return jax.nn.gelu(x, approximate=True)


def to_column(row):
    parts = []
    for at in range(0, row.shape[1], LANES):
        piece = jnp.broadcast_to(row[:, at : at + LANES], (LANES, LANES))
        parts.append(piece.T)
    return jnp.concatenate(parts, axis=0)


def kernel(
    sp, dp, value_hbm, ids_hbm, gain_hbm, mixing_ref, bias_hbm, gate_hbm, out_ref,
    value_ref, gate_ref, ids_ref, gain_ref, bias_ref,
    act_gate, vals, normed, ids, ids_row, ids_col, mix, res, ret, bias_col, extras, extras_in,
    in_sem, v_send, v_recv, i_send, i_recv, r_send, r_recv,
    mix_recv, across_send, core_send, fwd_send, own_sem, far_send, e_send, e_recv, far_ok,
):
    s, d = lax.axis_index("sp"), lax.axis_index("dp")
    tokens = value_ref.shape[0]
    block_len = mix.shape[1]
    per = block_len // tokens
    near = sp // 2
    blocks = near // per
    rows = mixing_ref.shape[0]
    part = rows // PARTS
    planes = dp // CORES
    half = s % per
    partner = d + 1 - 2 * (d % CORES)
    plane, core = d // CORES, d % CORES
    each = dp // per
    far = flip(s, sp - per, sp)
    level, levels = s // per, sp // per
    mid = (level == levels // 2 - 1) | (level == levels // 2)
    outer = (level < levels // 2 - 1) | (level > levels // 2)

    def across(step):
        return ((plane + step) % planes) * CORES + core

    barrier = pltpu.get_barrier_semaphore()
    for k in range(1, near):
        pl.semaphore_signal(barrier, inc=1, device_id={"sp": flip(s, k, sp)}, device_id_type=MESH)
    pl.semaphore_signal(barrier, inc=1, device_id={"dp": partner}, device_id_type=MESH)
    for step in range(1, planes):
        pl.semaphore_signal(barrier, inc=1, device_id={"dp": across(step)}, device_id_type=MESH)

    @pl.when(mid)
    def _():
        pl.semaphore_signal(barrier, inc=1, device_id={"sp": far}, device_id_type=MESH)

    loads = [
        pltpu.make_async_copy(src, dst, in_sem.at[n])
        for n, (src, dst) in enumerate([
            (value_hbm, value_ref), (ids_hbm, ids_ref), (gain_hbm, gain_ref),
            (bias_hbm, bias_ref), (gate_hbm, gate_ref),
        ])
    ]
    for load in loads:
        load.start()

    def chunk(which, origin, q):
        return mix.at[which, pl.ds(pl.multiple_of(origin * rows + q * part, part), part)]

    def part_copy(which, src, origin, q, where, sem):
        return pltpu.make_async_remote_copy(
            src_ref=src, dst_ref=chunk(which, origin, q), send_sem=sem,
            recv_sem=mix_recv.at[(which * dp + origin) * PARTS + q],
            device_id=where, device_id_type=MESH,
        )

    def held(which, q):
        return chunk(1, d, q) if which else mixing_ref.at[pl.ds(q * part, part)]

    def from_far(q):
        return part_copy(1, mixing_ref.at[pl.ds(q * part, part)], d, q, {"sp": far}, far_send.at[q])

    def to_plane(which, step, q):
        sem = across_send.at[(which * planes + step) * PARTS + q]
        return part_copy(which, held(which, q), d, q, {"dp": across(step)}, sem)

    def to_core(which, q):
        return part_copy(which, held(which, q), d, q, {"dp": partner}, core_send.at[which * PARTS + q])

    def pass_on(which, step, q):
        origin = across(planes - step)
        sem = fwd_send.at[(which * planes + step) * PARTS + q]
        return part_copy(which, chunk(which, origin, q), origin, q, {"dp": partner}, sem)

    def share(which, q):
        for step in range(1, planes):
            to_plane(which, step, q).start()
        to_core(which, q).start()

    def forward(which, q):
        for step in range(1, planes):
            pass_on(which, step, q).wait_recv()
            pass_on(which, step, q).start()

    def arrived(which, q):
        part_copy(which, held(which, q), partner, q, {"dp": partner}, core_send.at[0]).wait_recv()
        for step in range(1, planes):
            origin = across(planes - step)
            there = origin + 1 - 2 * (origin % CORES)
            part_copy(which, held(which, q), there, q, {"dp": partner}, core_send.at[0]).wait_recv()

    def extras_copy():
        return pltpu.make_async_remote_copy(
            src_ref=extras, dst_ref=extras_in, send_sem=e_send, recv_sem=e_recv,
            device_id={"sp": far}, device_id_type=MESH,
        )

    def head_of(owner, which):
        return flip(owner, which * (sp - per), sp)

    def lanes_of(head):
        return pl.ds(pl.multiple_of(head * HEAD_DIM, HEAD_DIM), HEAD_DIM)

    def value_copy(which, k, end):
        target = flip(s, k, sp)
        return pltpu.make_async_remote_copy(
            src_ref=value_ref.at[:, lanes_of(head_of(target, which))],
            dst_ref=vals.at[which * blocks + k // per, pl.ds(pl.multiple_of(end * tokens, tokens), tokens)],
            send_sem=v_send.at[which * near + k], recv_sem=v_recv.at[which * near + k],
            device_id={"sp": target}, device_id_type=MESH,
        )

    def id_copy(k, end):
        return pltpu.make_async_remote_copy(
            src_ref=ids_ref, dst_ref=ids.at[k // per, end],
            send_sem=i_send.at[k], recv_sem=i_recv.at[k],
            device_id={"sp": flip(s, k, sp)}, device_id_type=MESH,
        )

    def result_copy(which, k, q):
        target = flip(s, k, sp)
        at = (which * near + k) * PARTS + q
        return pltpu.make_async_remote_copy(
            src_ref=res.at[which * blocks + k // per, q, pl.ds((target % per) * each, each)],
            dst_ref=ret.at[which * near + k, q],
            send_sem=r_send.at[at], recv_sem=r_recv.at[at],
            device_id={"sp": target}, device_id_type=MESH,
        )

    pl.semaphore_wait(barrier, near - 1 + planes + mid.astype(jnp.int32))

    @pl.when(mid)
    def _():
        pl.semaphore_signal(far_ok, inc=1, device_id={"sp": far}, device_id_type=MESH)
        for q in range(PARTS):
            from_far(q).start()

    for q in range(PARTS):
        share(0, q)
    own = [pltpu.make_async_copy(mixing_ref.at[pl.ds(q * part, part)], chunk(0, d, q), own_sem.at[q]) for q in range(PARTS)]
    for copy in own:
        copy.start()
    loads[0].wait()
    loads[1].wait()

    def send_one(k, carry):
        value_copy(0, k, half).start()
        id_copy(k, half).start()
        return carry

    def send_more(k, carry):
        value_copy(1, k, half).start()
        return carry

    lax.fori_loop(1, near, send_one, 0)
    lax.fori_loop(1, near, send_more, 0)
    loads[2].wait()
    loads[3].wait()
    extras[:, :block_len] = bias_ref[...].astype(jnp.float32)
    extras[:, block_len:] = gain_ref[...].astype(jnp.float32)
    for which in (0, 1):
        vals[which * blocks, pl.ds(pl.multiple_of(half * tokens, tokens), tokens), :] = value_ref[:, lanes_of(head_of(s, which))]
    ids[0, half] = ids_ref[...]
    bias_col[0] = to_column(extras[:, :block_len])

    @pl.when(mid)
    def _():
        pl.semaphore_wait(far_ok, 1)
        for k in range(per, near, per):
            pl.semaphore_signal(far_ok, inc=1, device_id={"sp": flip(s, k, sp)}, device_id_type=MESH)
        extras_copy().start()

    @pl.when(outer)
    def _():
        pl.semaphore_wait(far_ok, 1)
        for q in range(PARTS):
            from_far(q).start()
        extras_copy().start()

    loads[4].wait()

    def gate_rows(n, carry):
        at = pl.ds(pl.multiple_of(n * LANES, LANES), LANES)
        act_gate[at, :] = gelu(gate_ref[at, :].astype(jnp.float32))
        return carry

    lax.fori_loop(0, tokens // LANES, gate_rows, 0)

    def norm_block(which, j):
        gain = (extras, extras_in)[which][:, block_len:]
        for i in range(per):
            k = j * per + i

            @pl.when(k > 0)
            def _():
                source_half = flip(s, k, sp) % per
                if which == 0:
                    id_copy(k, source_half).wait_recv()
                value_copy(which, k, source_half).wait_recv()

        n = which * blocks + j
        for at in range(0, block_len, ROW_STEP):
            act = gelu(vals[n, at : at + ROW_STEP, :].astype(jnp.float32))
            mean = jnp.mean(act * act, axis=-1, keepdims=True)
            normed[n, at : at + ROW_STEP, :] = (act * lax.rsqrt(mean + epsilon) * gain).astype(jnp.bfloat16)
        if which == 0:
            row = jnp.concatenate([ids[j, i] for i in range(per)], axis=1).astype(jnp.float32)
            ids_row[j] = row
            ids_col[j] = to_column(row).astype(jnp.bfloat16)

    def norm_blocks(which, first, last):
        def body(j, carry):
            norm_block(which, j)
            return carry

        lax.fori_loop(first, last, body, 0)

    zero = jnp.zeros((), jnp.bfloat16)

    def mix_part(which, q):
        def body(j, carry):
            n = which * blocks + j
            row_b = ids_row[j].astype(jnp.bfloat16)
            right = normed[n]
            tall = []
            for origin in range(dp):
                at = origin * rows + q * part
                col = ids_col[j, pl.ds(pl.multiple_of(at, part), part), :]
                wide = []
                for c in range(0, block_len, LANES):
                    same = col == row_b[:, c : c + LANES]
                    piece = mix[which, pl.ds(pl.multiple_of(at, part), part), c : c + LANES]
                    wide.append(jnp.where(same, piece, zero))
                tall.append(jnp.concatenate(wide, axis=1))
            summed = jnp.dot(jnp.concatenate(tall, axis=0), right, preferred_element_type=jnp.float32)
            for origin in range(dp):
                at = origin * rows + q * part
                bias = bias_col[which, pl.ds(pl.multiple_of(at, part), part), :]
                res[n, q, origin] = (summed[origin * part : (origin + 1) * part] + bias).astype(jnp.bfloat16)
            for i in range(per):
                k = j * per + i

                @pl.when(k > 0)
                def _():
                    result_copy(which, k, q).start()
            return carry

        lax.fori_loop(0, blocks, body, 0)

    forward(0, 0)
    norm_blocks(0, 0, blocks // 2)
    forward(0, 1)
    norm_blocks(0, blocks // 2, blocks)
    forward(0, 2)
    extras_copy().wait_recv()
    bias_col[1] = to_column(extras_in[:, :block_len])
    norm_blocks(1, 0, blocks // 2)
    forward(0, 3)
    norm_blocks(1, blocks // 2, blocks)

    def relay(q):
        from_far(q).wait_recv()
        share(1, q)

    @pl.when(mid)
    def _():
        for q in range(PARTS):
            relay(q)

    for q in range(PARTS):
        own[q].wait()
        arrived(0, q)
        mix_part(0, q)

    for n in range(PARTS + 2):
        if n < PARTS:
            @pl.when(outer)
            def _():
                relay(n)
        if n >= 2:
            arrived(1, n - 2)
            mix_part(1, n - 2)
        if 1 <= n < PARTS + 1:
            forward(1, n - 1)

    def finish_one(which, k, source, n):
        lanes = lanes_of(head_of(flip(s, k, sp), which))
        for q in range(PARTS):
            for e in range(each):
                at = e * rows + q * part
                got = source(q, e).astype(jnp.float32)
                out_ref[at : at + part, lanes] = (act_gate[at : at + part, lanes] * got).astype(jnp.bfloat16)

    for which in (0, 1):
        finish_one(which, 0, lambda q, e: res[which * blocks, q, half * each + e], 0)

        def finish(k, carry):
            for q in range(PARTS):
                result_copy(which, k, q).wait_recv()
            finish_one(which, k, lambda q, e: ret[which * near + k, q, e], 0)
            return carry

        lax.fori_loop(1, near, finish, 0)

    def drain(k, carry):
        id_copy(k, half).wait_send()
        for which in (0, 1):
            value_copy(which, k, half).wait_send()
            for q in range(PARTS):
                result_copy(which, k, q).wait_send()
        return carry

    lax.fori_loop(1, near, drain, 0)
    extras_copy().wait_send()
    for q in range(PARTS):
        from_far(q).wait_send()
        for which in (0, 1):
            to_core(which, q).wait_send()
            for step in range(1, planes):
                to_plane(which, step, q).wait_send()
                pass_on(which, step, q).wait_send()


def per_device(gate_in, value_in, segments, value_gain, mixing, mixing_bias):
    sp, dp = lax.axis_size("sp"), lax.axis_size("dp")
    sequences, tokens, width = value_in.shape
    heads_here, rows, block_len = mixing.shape
    assert sequences == 1 and heads_here == 1
    per = block_len // tokens
    near = sp // 2
    blocks = near // per
    planes = dp // CORES
    part = rows // PARTS
    bf16, f32 = jnp.bfloat16, jnp.float32
    dma = pltpu.SemaphoreType.DMA
    vmem, anywhere = pl.BlockSpec(memory_space=pltpu.VMEM), pl.BlockSpec(memory_space=pl.ANY)
    out = pl.pallas_call(
        functools.partial(kernel, sp, dp),
        out_shape=jax.ShapeDtypeStruct((tokens, width), bf16),
        in_specs=[anywhere] * 6,
        out_specs=vmem,
        scratch_shapes=[
            pltpu.VMEM((tokens, width), bf16),
            pltpu.VMEM((tokens, width), bf16),
            pltpu.VMEM((1, tokens), jnp.int32),
            pltpu.VMEM((1, HEAD_DIM), bf16),
            pltpu.VMEM((1, block_len), bf16),
            pltpu.VMEM((tokens, width), f32),
            pltpu.VMEM((2 * blocks, block_len, HEAD_DIM), bf16),
            pltpu.VMEM((2 * blocks, block_len, HEAD_DIM), bf16),
            pltpu.VMEM((blocks, per, 1, tokens), jnp.int32),
            pltpu.VMEM((blocks, 1, block_len), f32),
            pltpu.VMEM((blocks, block_len, LANES), bf16),
            pltpu.VMEM((2, block_len, block_len), bf16),
            pltpu.VMEM((2 * blocks, PARTS, dp, part, HEAD_DIM), bf16),
            pltpu.VMEM((sp, PARTS, dp // per, part, HEAD_DIM), bf16),
            pltpu.VMEM((2, block_len, LANES), f32),
            pltpu.VMEM((1, block_len + HEAD_DIM), f32),
            pltpu.VMEM((1, block_len + HEAD_DIM), f32),
            dma((5,)), dma((sp,)), dma((sp,)), dma((sp,)), dma((sp,)),
            dma((sp * PARTS,)), dma((sp * PARTS,)),
            dma((2 * dp * PARTS,)), dma((2 * planes * PARTS,)), dma((2 * PARTS,)),
            dma((2 * planes * PARTS,)), dma((PARTS,)), dma((PARTS,)), dma, dma,
            pltpu.SemaphoreType.REGULAR,
        ],
        compiler_params=pltpu.CompilerParams(
            collective_id=0, has_side_effects=True, vmem_limit_bytes=60 * 1024 * 1024
        ),
    )(
        value_in.reshape(tokens, width),
        segments,
        value_gain.reshape(1, HEAD_DIM),
        mixing.reshape(rows, block_len),
        mixing_bias,
        gate_in.reshape(tokens, width),
    )
    return out.reshape(sequences, tokens, width)


def solution(mesh):
    return jax.shard_map(
        per_device,
        mesh=mesh,
        in_specs=(
            P("dp", "sp", None),
            P("dp", "sp", None),
            P("dp", "sp"),
            P("sp"),
            P("sp", "dp", None),
            P("sp", None),
        ),
        out_specs=P("dp", "sp", None),
        check_vma=False,
    )
```

```python
import functools

import jax
import jax.numpy as jnp
from jax import lax
from jax.experimental import pallas as pl
from jax.experimental.pallas import tpu as pltpu
from jax.sharding import PartitionSpec as P

HEAD_DIM = 128
CORES = 2
LANES = 128
ROW_STEP = 256
PARTS = 4
MESH = pl.DeviceIdType.MESH

epsilon = 1e-06


def flip(a, b, count):
    total, bit = 0, 1
    while bit < count:
        total = total + ((a // bit + b // bit) % 2) * bit
        bit *= 2
    return total


def gelu(x):
    return jax.nn.gelu(x, approximate=True)


def to_column(row):
    parts = []
    for at in range(0, row.shape[1], LANES):
        piece = jnp.broadcast_to(row[:, at : at + LANES], (LANES, LANES))
        parts.append(piece.T)
    return jnp.concatenate(parts, axis=0)


def kernel(
    sp, dp, value_hbm, ids_hbm, gain_hbm, mixing_ref, bias_hbm, gate_hbm, out_ref,
    value_ref, gate_ref, ids_ref, gain_ref, bias_ref,
    act_gate, vals, normed, ids, ids_row, ids_col, mix, res, ret, bias_col, extras, extras_in,
    in_sem, v_send, v_recv, i_send, i_recv, r_send, r_recv,
    mix_recv, across_send, core_send, fwd_send, own_sem, far_send, e_send, e_recv, far_ok,
):
    s, d = lax.axis_index("sp"), lax.axis_index("dp")
    tokens = value_ref.shape[0]
    block_len = mix.shape[1]
    per = block_len // tokens
    near = sp // 2
    blocks = near // per
    rows = mixing_ref.shape[0]
    part = rows // PARTS
    planes = dp // CORES
    half = s % per
    partner = d + 1 - 2 * (d % CORES)
    plane, core = d // CORES, d % CORES
    each = dp // per
    far = flip(s, sp - per, sp)
    level, levels = s // per, sp // per
    mid = (level == levels // 2 - 1) | (level == levels // 2)
    outer = (level < levels // 2 - 1) | (level > levels // 2)

    def across(step):
        return ((plane + step) % planes) * CORES + core

    barrier = pltpu.get_barrier_semaphore()
    for k in range(1, near):
        pl.semaphore_signal(barrier, inc=1, device_id={"sp": flip(s, k, sp)}, device_id_type=MESH)
    pl.semaphore_signal(barrier, inc=1, device_id={"dp": partner}, device_id_type=MESH)
    for step in range(1, planes):
        pl.semaphore_signal(barrier, inc=1, device_id={"dp": across(step)}, device_id_type=MESH)

    @pl.when(mid)
    def _():
        pl.semaphore_signal(barrier, inc=1, device_id={"sp": far}, device_id_type=MESH)

    loads = [
        pltpu.make_async_copy(src, dst, in_sem.at[n])
        for n, (src, dst) in enumerate([
            (value_hbm, value_ref), (ids_hbm, ids_ref), (gain_hbm, gain_ref),
            (bias_hbm, bias_ref), (gate_hbm, gate_ref),
        ])
    ]
    for load in loads:
        load.start()

    count = (1, PARTS)

    def chunk(which, origin, q):
        size = rows // count[which]
        return mix.at[which, pl.ds(pl.multiple_of(origin * rows + q * size, size), size)]

    def part_copy(which, src, origin, q, where, sem):
        return pltpu.make_async_remote_copy(
            src_ref=src, dst_ref=chunk(which, origin, q), send_sem=sem,
            recv_sem=mix_recv.at[(which * dp + origin) * PARTS + q],
            device_id=where, device_id_type=MESH,
        )

    def held(which, q):
        return chunk(1, d, q) if which else mixing_ref

    def from_far(q):
        return part_copy(1, mixing_ref.at[pl.ds(q * part, part)], d, q, {"sp": far}, far_send.at[q])

    def to_plane(which, step, q):
        sem = across_send.at[(which * planes + step) * PARTS + q]
        return part_copy(which, held(which, q), d, q, {"dp": across(step)}, sem)

    def to_core(which, q):
        return part_copy(which, held(which, q), d, q, {"dp": partner}, core_send.at[which * PARTS + q])

    def pass_on(which, step, q):
        origin = across(planes - step)
        sem = fwd_send.at[(which * planes + step) * PARTS + q]
        return part_copy(which, chunk(which, origin, q), origin, q, {"dp": partner}, sem)

    def share(which, q):
        for step in range(1, planes):
            to_plane(which, step, q).start()
        to_core(which, q).start()

    def forward(which, q):
        for step in range(1, planes):
            pass_on(which, step, q).wait_recv()
            pass_on(which, step, q).start()

    def arrived(which, q):
        part_copy(which, held(which, q), partner, q, {"dp": partner}, core_send.at[0]).wait_recv()
        for step in range(1, planes):
            origin = across(planes - step)
            there = origin + 1 - 2 * (origin % CORES)
            part_copy(which, held(which, q), there, q, {"dp": partner}, core_send.at[0]).wait_recv()

    def extras_copy():
        return pltpu.make_async_remote_copy(
            src_ref=extras, dst_ref=extras_in, send_sem=e_send, recv_sem=e_recv,
            device_id={"sp": far}, device_id_type=MESH,
        )

    def head_of(owner, which):
        return flip(owner, which * (sp - per), sp)

    def lanes_of(head):
        return pl.ds(pl.multiple_of(head * HEAD_DIM, HEAD_DIM), HEAD_DIM)

    def value_copy(which, k, end):
        target = flip(s, k, sp)
        return pltpu.make_async_remote_copy(
            src_ref=value_ref.at[:, lanes_of(head_of(target, which))],
            dst_ref=vals.at[which * blocks + k // per, pl.ds(pl.multiple_of(end * tokens, tokens), tokens)],
            send_sem=v_send.at[which * near + k], recv_sem=v_recv.at[which * near + k],
            device_id={"sp": target}, device_id_type=MESH,
        )

    def id_copy(k, end):
        return pltpu.make_async_remote_copy(
            src_ref=ids_ref, dst_ref=ids.at[k // per, end],
            send_sem=i_send.at[k], recv_sem=i_recv.at[k],
            device_id={"sp": flip(s, k, sp)}, device_id_type=MESH,
        )

    def result_copy(which, k, q):
        target = flip(s, k, sp)
        at = (which * near + k) * PARTS + q
        return pltpu.make_async_remote_copy(
            src_ref=res.at[which * blocks + k // per, q, pl.ds((target % per) * each, each)],
            dst_ref=ret.at[which * near + k, q],
            send_sem=r_send.at[at], recv_sem=r_recv.at[at],
            device_id={"sp": target}, device_id_type=MESH,
        )

    loads[2].wait()
    loads[3].wait()
    extras[:, :block_len] = bias_ref[...].astype(jnp.float32)
    extras[:, block_len:] = gain_ref[...].astype(jnp.float32)
    pl.semaphore_wait(barrier, near - 1 + planes + mid.astype(jnp.int32))

    @pl.when(mid)
    def _():
        pl.semaphore_signal(far_ok, inc=1, device_id={"sp": far}, device_id_type=MESH)
        extras_copy().start()
        for q in range(PARTS):
            from_far(q).start()

    share(0, 0)
    own = pltpu.make_async_copy(mixing_ref, chunk(0, d, 0), own_sem)
    own.start()
    loads[0].wait()
    loads[1].wait()

    def send_one(k, carry):
        value_copy(0, k, half).start()
        id_copy(k, half).start()
        return carry

    def send_more(k, carry):
        value_copy(1, k, half).start()
        return carry

    lax.fori_loop(1, near, send_one, 0)
    lax.fori_loop(1, near, send_more, 0)
    for which in (0, 1):
        vals[which * blocks, pl.ds(pl.multiple_of(half * tokens, tokens), tokens), :] = value_ref[:, lanes_of(head_of(s, which))]
    ids[0, half] = ids_ref[...]
    bias_col[0] = to_column(extras[:, :block_len])

    @pl.when(mid)
    def _():
        pl.semaphore_wait(far_ok, 1)
        for k in range(per, near, per):
            pl.semaphore_signal(far_ok, inc=1, device_id={"sp": flip(s, k, sp)}, device_id_type=MESH)

    @pl.when(outer)
    def _():
        pl.semaphore_wait(far_ok, 1)
        extras_copy().start()
        for q in range(PARTS):
            from_far(q).start()

    loads[4].wait()

    def gate_rows(n, carry):
        at = pl.ds(pl.multiple_of(n * LANES, LANES), LANES)
        act_gate[at, :] = gelu(gate_ref[at, :].astype(jnp.float32))
        return carry

    lax.fori_loop(0, tokens // LANES, gate_rows, 0)

    def norm_block(which, j):
        gain = (extras, extras_in)[which][:, block_len:]
        for i in range(per):
            k = j * per + i

            @pl.when(k > 0)
            def _():
                source_half = flip(s, k, sp) % per
                if which == 0:
                    id_copy(k, source_half).wait_recv()
                value_copy(which, k, source_half).wait_recv()

        n = which * blocks + j
        for at in range(0, block_len, ROW_STEP):
            act = gelu(vals[n, at : at + ROW_STEP, :].astype(jnp.float32))
            mean = jnp.mean(act * act, axis=-1, keepdims=True)
            normed[n, at : at + ROW_STEP, :] = (act * lax.rsqrt(mean + epsilon) * gain).astype(jnp.bfloat16)
        if which == 0:
            row = jnp.concatenate([ids[j, i] for i in range(per)], axis=1).astype(jnp.float32)
            ids_row[j] = row
            ids_col[j] = to_column(row).astype(jnp.bfloat16)

    def norm_blocks(which, first, last):
        def body(j, carry):
            norm_block(which, j)
            return carry

        lax.fori_loop(first, last, body, 0)

    zero = jnp.zeros((), jnp.bfloat16)

    def mix_part(which, q):
        def body(j, carry):
            n = which * blocks + j
            row_b = ids_row[j].astype(jnp.bfloat16)
            right = normed[n]
            tall = []
            for origin in range(dp):
                at = origin * rows + q * part
                col = ids_col[j, pl.ds(pl.multiple_of(at, part), part), :]
                wide = []
                for c in range(0, block_len, LANES):
                    same = col == row_b[:, c : c + LANES]
                    piece = mix[which, pl.ds(pl.multiple_of(at, part), part), c : c + LANES]
                    wide.append(jnp.where(same, piece, zero))
                tall.append(jnp.concatenate(wide, axis=1))
            summed = jnp.dot(jnp.concatenate(tall, axis=0), right, preferred_element_type=jnp.float32)
            for origin in range(dp):
                at = origin * rows + q * part
                bias = bias_col[which, pl.ds(pl.multiple_of(at, part), part), :]
                res[n, q, origin] = (summed[origin * part : (origin + 1) * part] + bias).astype(jnp.bfloat16)
            for i in range(per):
                k = j * per + i

                @pl.when(k > 0)
                def _():
                    result_copy(which, k, q).start()
            return carry

        lax.fori_loop(0, blocks, body, 0)

    norm_blocks(0, 0, blocks)

    def relay(q):
        from_far(q).wait_recv()
        share(1, q)

    @pl.when(mid)
    def _():
        for q in range(PARTS):
            relay(q)

    forward(0, 0)
    own.wait()
    arrived(0, 0)
    for q in range(PARTS):
        mix_part(0, q)

    for n in range(PARTS + 2):
        if n < PARTS:
            @pl.when(outer)
            def _():
                relay(n)
        if n == 0:
            extras_copy().wait_recv()
            bias_col[1] = to_column(extras_in[:, :block_len])
            norm_blocks(1, 0, blocks)
        if n >= 2:
            arrived(1, n - 2)
            mix_part(1, n - 2)
        if 1 <= n < PARTS + 1:
            forward(1, n - 1)

    def finish_one(which, k, source, n):
        lanes = lanes_of(head_of(flip(s, k, sp), which))
        for q in range(PARTS):
            for e in range(each):
                at = e * rows + q * part
                got = source(q, e).astype(jnp.float32)
                out_ref[at : at + part, lanes] = (act_gate[at : at + part, lanes] * got).astype(jnp.bfloat16)

    for which in (0, 1):
        finish_one(which, 0, lambda q, e: res[which * blocks, q, half * each + e], 0)

        def finish(k, carry):
            for q in range(PARTS):
                result_copy(which, k, q).wait_recv()
            finish_one(which, k, lambda q, e: ret[which * near + k, q, e], 0)
            return carry

        lax.fori_loop(1, near, finish, 0)

    def drain(k, carry):
        id_copy(k, half).wait_send()
        for which in (0, 1):
            value_copy(which, k, half).wait_send()
            for q in range(PARTS):
                result_copy(which, k, q).wait_send()
        return carry

    lax.fori_loop(1, near, drain, 0)
    extras_copy().wait_send()
    for q in range(PARTS):
        from_far(q).wait_send()
    for which in (0, 1):
        for q in range(count[which]):
            to_core(which, q).wait_send()
            for step in range(1, planes):
                to_plane(which, step, q).wait_send()
                pass_on(which, step, q).wait_send()


def per_device(gate_in, value_in, segments, value_gain, mixing, mixing_bias):
    sp, dp = lax.axis_size("sp"), lax.axis_size("dp")
    sequences, tokens, width = value_in.shape
    heads_here, rows, block_len = mixing.shape
    assert sequences == 1 and heads_here == 1
    per = block_len // tokens
    near = sp // 2
    blocks = near // per
    planes = dp // CORES
    part = rows // PARTS
    bf16, f32 = jnp.bfloat16, jnp.float32
    dma = pltpu.SemaphoreType.DMA
    vmem, anywhere = pl.BlockSpec(memory_space=pltpu.VMEM), pl.BlockSpec(memory_space=pl.ANY)
    out = pl.pallas_call(
        functools.partial(kernel, sp, dp),
        out_shape=jax.ShapeDtypeStruct((tokens, width), bf16),
        in_specs=[anywhere] * 6,
        out_specs=vmem,
        scratch_shapes=[
            pltpu.VMEM((tokens, width), bf16),
            pltpu.VMEM((tokens, width), bf16),
            pltpu.VMEM((1, tokens), jnp.int32),
            pltpu.VMEM((1, HEAD_DIM), bf16),
            pltpu.VMEM((1, block_len), bf16),
            pltpu.VMEM((tokens, width), f32),
            pltpu.VMEM((2 * blocks, block_len, HEAD_DIM), bf16),
            pltpu.VMEM((2 * blocks, block_len, HEAD_DIM), bf16),
            pltpu.VMEM((blocks, per, 1, tokens), jnp.int32),
            pltpu.VMEM((blocks, 1, block_len), f32),
            pltpu.VMEM((blocks, block_len, LANES), bf16),
            pltpu.VMEM((2, block_len, block_len), bf16),
            pltpu.VMEM((2 * blocks, PARTS, dp, part, HEAD_DIM), bf16),
            pltpu.VMEM((sp, PARTS, dp // per, part, HEAD_DIM), bf16),
            pltpu.VMEM((2, block_len, LANES), f32),
            pltpu.VMEM((1, block_len + HEAD_DIM), f32),
            pltpu.VMEM((1, block_len + HEAD_DIM), f32),
            dma((5,)), dma((sp,)), dma((sp,)), dma((sp,)), dma((sp,)),
            dma((sp * PARTS,)), dma((sp * PARTS,)),
            dma((2 * dp * PARTS,)), dma((2 * planes * PARTS,)), dma((2 * PARTS,)),
            dma((2 * planes * PARTS,)), dma, dma((PARTS,)), dma, dma,
            pltpu.SemaphoreType.REGULAR,
        ],
        compiler_params=pltpu.CompilerParams(
            collective_id=0, has_side_effects=True, vmem_limit_bytes=60 * 1024 * 1024
        ),
    )(
        value_in.reshape(tokens, width),
        segments,
        value_gain.reshape(1, HEAD_DIM),
        mixing.reshape(rows, block_len),
        mixing_bias,
        gate_in.reshape(tokens, width),
    )
    return out.reshape(sequences, tokens, width)


def solution(mesh):
    return jax.shard_map(
        per_device,
        mesh=mesh,
        in_specs=(
            P("dp", "sp", None),
            P("dp", "sp", None),
            P("dp", "sp"),
            P("sp"),
            P("sp", "dp", None),
            P("sp", None),
        ),
        out_specs=P("dp", "sp", None),
        check_vma=False,
    )
```

```python
import functools

import jax
import jax.numpy as jnp
from jax import lax
from jax.experimental import pallas as pl
from jax.experimental.pallas import tpu as pltpu
from jax.sharding import PartitionSpec as P

HEAD_DIM = 128
CORES = 2
LANES = 128
ROW_STEP = 256
PARTS = 4
MESH = pl.DeviceIdType.MESH

epsilon = 1e-06


def flip(a, b, count):
    total, bit = 0, 1
    while bit < count:
        total = total + ((a // bit + b // bit) % 2) * bit
        bit *= 2
    return total


def gelu(x):
    return jax.nn.gelu(x, approximate=True)


def to_column(row):
    parts = []
    for at in range(0, row.shape[1], LANES):
        piece = jnp.broadcast_to(row[:, at : at + LANES], (LANES, LANES))
        parts.append(piece.T)
    return jnp.concatenate(parts, axis=0)


def kernel(
    sp, dp, value_hbm, ids_hbm, gain_hbm, mixing_ref, bias_hbm, mixed_ref,
    value_ref, ids_ref, gain_ref, bias_ref,
    vals, normed, ids, ids_row, ids_col, mix, res, bias_col, extras, extras_in,
    in_sem, v_send, v_recv, i_send, i_recv, r_send, r_recv,
    mix_recv, across_send, core_send, fwd_send, own_sem, far_send, e_send, e_recv, far_ok, keep_sem,
):
    s, d = lax.axis_index("sp"), lax.axis_index("dp")
    tokens = value_ref.shape[0]
    block_len = mix.shape[1]
    per = block_len // tokens
    near = sp // 2
    blocks = near // per
    rows = mixing_ref.shape[0]
    part = rows // PARTS
    planes = dp // CORES
    half = s % per
    partner = d + 1 - 2 * (d % CORES)
    plane, core = d // CORES, d % CORES
    each = dp // per
    far = flip(s, sp - per, sp)
    level, levels = s // per, sp // per
    mid = (level == levels // 2 - 1) | (level == levels // 2)
    outer = (level < levels // 2 - 1) | (level > levels // 2)

    def across(step):
        return ((plane + step) % planes) * CORES + core

    barrier = pltpu.get_barrier_semaphore()
    for k in range(1, near):
        pl.semaphore_signal(barrier, inc=1, device_id={"sp": flip(s, k, sp)}, device_id_type=MESH)
    pl.semaphore_signal(barrier, inc=1, device_id={"dp": partner}, device_id_type=MESH)
    for step in range(1, planes):
        pl.semaphore_signal(barrier, inc=1, device_id={"dp": across(step)}, device_id_type=MESH)

    @pl.when(mid)
    def _():
        pl.semaphore_signal(barrier, inc=1, device_id={"sp": far}, device_id_type=MESH)

    loads = [
        pltpu.make_async_copy(src, dst, in_sem.at[n])
        for n, (src, dst) in enumerate([
            (value_hbm, value_ref), (ids_hbm, ids_ref), (gain_hbm, gain_ref),
            (bias_hbm, bias_ref),
        ])
    ]
    for load in loads:
        load.start()

    count = (1, PARTS)

    def chunk(which, origin, q):
        size = rows // count[which]
        return mix.at[which, pl.ds(pl.multiple_of(origin * rows + q * size, size), size)]

    def part_copy(which, src, origin, q, where, sem):
        return pltpu.make_async_remote_copy(
            src_ref=src, dst_ref=chunk(which, origin, q), send_sem=sem,
            recv_sem=mix_recv.at[(which * dp + origin) * PARTS + q],
            device_id=where, device_id_type=MESH,
        )

    def held(which, q):
        return chunk(1, d, q) if which else mixing_ref

    def from_far(q):
        return part_copy(1, mixing_ref.at[pl.ds(q * part, part)], d, q, {"sp": far}, far_send.at[q])

    def to_plane(which, step, q):
        sem = across_send.at[(which * planes + step) * PARTS + q]
        return part_copy(which, held(which, q), d, q, {"dp": across(step)}, sem)

    def to_core(which, q):
        return part_copy(which, held(which, q), d, q, {"dp": partner}, core_send.at[which * PARTS + q])

    def pass_on(which, step, q):
        origin = across(planes - step)
        sem = fwd_send.at[(which * planes + step) * PARTS + q]
        return part_copy(which, chunk(which, origin, q), origin, q, {"dp": partner}, sem)

    def share(which, q):
        for step in range(1, planes):
            to_plane(which, step, q).start()
        to_core(which, q).start()

    def forward(which, q):
        for step in range(1, planes):
            pass_on(which, step, q).wait_recv()
            pass_on(which, step, q).start()

    def arrived(which, q):
        part_copy(which, held(which, q), partner, q, {"dp": partner}, core_send.at[0]).wait_recv()
        for step in range(1, planes):
            origin = across(planes - step)
            there = origin + 1 - 2 * (origin % CORES)
            part_copy(which, held(which, q), there, q, {"dp": partner}, core_send.at[0]).wait_recv()

    def extras_copy():
        return pltpu.make_async_remote_copy(
            src_ref=extras, dst_ref=extras_in, send_sem=e_send, recv_sem=e_recv,
            device_id={"sp": far}, device_id_type=MESH,
        )

    def head_of(owner, which):
        return flip(owner, which * (sp - per), sp)

    def lanes_of(head):
        return pl.ds(pl.multiple_of(head * HEAD_DIM, HEAD_DIM), HEAD_DIM)

    def value_copy(which, k, end):
        target = flip(s, k, sp)
        return pltpu.make_async_remote_copy(
            src_ref=value_ref.at[:, lanes_of(head_of(target, which))],
            dst_ref=vals.at[which * blocks + k // per, pl.ds(pl.multiple_of(end * tokens, tokens), tokens)],
            send_sem=v_send.at[which * near + k], recv_sem=v_recv.at[which * near + k],
            device_id={"sp": target}, device_id_type=MESH,
        )

    def id_copy(k, end):
        return pltpu.make_async_remote_copy(
            src_ref=ids_ref, dst_ref=ids.at[k // per, end],
            send_sem=i_send.at[k], recv_sem=i_recv.at[k],
            device_id={"sp": flip(s, k, sp)}, device_id_type=MESH,
        )

    def place(owner, which, q):
        return mixed_ref.at[:, q, :, lanes_of(head_of(owner, which))]

    def keep_copy(which, q):
        return pltpu.make_async_copy(
            res.at[which * blocks, q, pl.ds(half * each, each)],
            place(s, which, q), keep_sem.at[which * PARTS + q],
        )

    def result_copy(which, k, q):
        target = flip(s, k, sp)
        at = (which * near + k) * PARTS + q
        return pltpu.make_async_remote_copy(
            src_ref=res.at[which * blocks + k // per, q, pl.ds((target % per) * each, each)],
            dst_ref=place(s, which, q),
            send_sem=r_send.at[at], recv_sem=r_recv.at[at],
            device_id={"sp": target}, device_id_type=MESH,
        )

    loads[2].wait()
    loads[3].wait()
    extras[:, :block_len] = bias_ref[...].astype(jnp.float32)
    extras[:, block_len:] = gain_ref[...].astype(jnp.float32)
    pl.semaphore_wait(barrier, near - 1 + planes + mid.astype(jnp.int32))

    @pl.when(mid)
    def _():
        pl.semaphore_signal(far_ok, inc=1, device_id={"sp": far}, device_id_type=MESH)
        extras_copy().start()
        for q in range(PARTS):
            from_far(q).start()

    share(0, 0)
    own = pltpu.make_async_copy(mixing_ref, chunk(0, d, 0), own_sem)
    own.start()
    loads[0].wait()
    loads[1].wait()

    def send_one(k, carry):
        value_copy(0, k, half).start()
        id_copy(k, half).start()
        return carry

    def send_more(k, carry):
        value_copy(1, k, half).start()
        return carry

    lax.fori_loop(1, near, send_one, 0)
    lax.fori_loop(1, near, send_more, 0)
    for which in (0, 1):
        vals[which * blocks, pl.ds(pl.multiple_of(half * tokens, tokens), tokens), :] = value_ref[:, lanes_of(head_of(s, which))]
    ids[0, half] = ids_ref[...]
    bias_col[0] = to_column(extras[:, :block_len])

    @pl.when(mid)
    def _():
        pl.semaphore_wait(far_ok, 1)
        for k in range(per, near, per):
            pl.semaphore_signal(far_ok, inc=1, device_id={"sp": flip(s, k, sp)}, device_id_type=MESH)

    @pl.when(outer)
    def _():
        pl.semaphore_wait(far_ok, 1)
        extras_copy().start()
        for q in range(PARTS):
            from_far(q).start()

    def norm_block(which, j):
        gain = (extras, extras_in)[which][:, block_len:]
        for i in range(per):
            k = j * per + i

            @pl.when(k > 0)
            def _():
                source_half = flip(s, k, sp) % per
                if which == 0:
                    id_copy(k, source_half).wait_recv()
                value_copy(which, k, source_half).wait_recv()

        n = which * blocks + j
        for at in range(0, block_len, ROW_STEP):
            act = gelu(vals[n, at : at + ROW_STEP, :].astype(jnp.float32))
            mean = jnp.mean(act * act, axis=-1, keepdims=True)
            normed[n, at : at + ROW_STEP, :] = (act * lax.rsqrt(mean + epsilon) * gain).astype(jnp.bfloat16)
        if which == 0:
            row = jnp.concatenate([ids[j, i] for i in range(per)], axis=1).astype(jnp.float32)
            ids_row[j] = row
            ids_col[j] = to_column(row).astype(jnp.bfloat16)

    def norm_blocks(which, first, last):
        def body(j, carry):
            norm_block(which, j)
            return carry

        lax.fori_loop(first, last, body, 0)

    zero = jnp.zeros((), jnp.bfloat16)

    def mix_part(which, q, first=0, last=blocks):
        def body(m, carry):
            j = last - 1 - m
            n = which * blocks + j
            row_b = ids_row[j].astype(jnp.bfloat16)
            right = normed[n]
            tall = []
            for origin in range(dp):
                at = origin * rows + q * part
                col = ids_col[j, pl.ds(pl.multiple_of(at, part), part), :]
                wide = []
                for c in range(0, block_len, LANES):
                    same = col == row_b[:, c : c + LANES]
                    piece = mix[which, pl.ds(pl.multiple_of(at, part), part), c : c + LANES]
                    wide.append(jnp.where(same, piece, zero))
                tall.append(jnp.concatenate(wide, axis=1))
            summed = jnp.dot(jnp.concatenate(tall, axis=0), right, preferred_element_type=jnp.float32)
            for origin in range(dp):
                at = origin * rows + q * part
                bias = bias_col[which, pl.ds(pl.multiple_of(at, part), part), :]
                res[n, q, origin] = (summed[origin * part : (origin + 1) * part] + bias).astype(jnp.bfloat16)
            for i in range(per):
                k = j * per + i

                @pl.when(k > 0)
                def _():
                    result_copy(which, k, q).start()

                @pl.when(k == 0)
                def _():
                    keep_copy(which, q).start()
            return carry

        lax.fori_loop(0, last - first, body, 0)

    norm_blocks(0, 0, blocks)

    def relay(q):
        from_far(q).wait_recv()
        share(1, q)

    def near_parts(first, last):
        def body(q, carry):
            mix_part(0, q, first, last)
            return carry

        lax.fori_loop(0, PARTS, body, 0)

    def near_here():
        forward(0, 0)
        own.wait()
        arrived(0, 0)
        near_parts(0, blocks)

    def far_values():
        extras_copy().wait_recv()
        bias_col[1] = to_column(extras_in[:, :block_len])
        norm_blocks(1, 0, blocks)

    def far_part(q):
        arrived(1, q)
        mix_part(1, q)

    @pl.when(mid)
    def _():
        relay(0)
        relay(1)
        near_here()
        far_values()
        for q in range(PARTS):
            forward(1, q)
            if q + 2 < PARTS:
                relay(q + 2)
            if q > 0:
                far_part(q - 1)
        far_part(PARTS - 1)

    @pl.when(outer)
    def _():
        near_here()
        relay(0)
        far_values()
        relay(1)
        forward(1, 0)
        for q in range(2, PARTS):
            relay(q)
            forward(1, q - 1)
            far_part(q - 2)
        far_part(PARTS - 2)
        forward(1, PARTS - 1)
        far_part(PARTS - 1)

    for which in (0, 1):
        for q in range(PARTS):
            keep_copy(which, q).wait()

        def collect(k, carry):
            for q in range(PARTS):
                result_copy(which, k, q).wait_recv()
            return carry

        lax.fori_loop(1, near, collect, 0)

    def drain(k, carry):
        id_copy(k, half).wait_send()
        for which in (0, 1):
            value_copy(which, k, half).wait_send()
            for q in range(PARTS):
                result_copy(which, k, q).wait_send()
        return carry

    lax.fori_loop(1, near, drain, 0)
    extras_copy().wait_send()
    for q in range(PARTS):
        from_far(q).wait_send()
    for which in (0, 1):
        for q in range(count[which]):
            to_core(which, q).wait_send()
            for step in range(1, planes):
                to_plane(which, step, q).wait_send()
                pass_on(which, step, q).wait_send()


def per_device(gate_in, value_in, segments, value_gain, mixing, mixing_bias):
    sp, dp = lax.axis_size("sp"), lax.axis_size("dp")
    sequences, tokens, width = value_in.shape
    heads_here, rows, block_len = mixing.shape
    assert sequences == 1 and heads_here == 1
    per = block_len // tokens
    near = sp // 2
    blocks = near // per
    planes = dp // CORES
    part = rows // PARTS
    bf16, f32 = jnp.bfloat16, jnp.float32
    dma = pltpu.SemaphoreType.DMA
    vmem, anywhere = pl.BlockSpec(memory_space=pltpu.VMEM), pl.BlockSpec(memory_space=pl.ANY)
    mixed = pl.pallas_call(
        functools.partial(kernel, sp, dp),
        out_shape=jax.ShapeDtypeStruct((dp // per, PARTS, part, width), bf16),
        in_specs=[anywhere] * 5,
        out_specs=anywhere,
        scratch_shapes=[
            pltpu.VMEM((tokens, width), bf16),
            pltpu.VMEM((1, tokens), jnp.int32),
            pltpu.VMEM((1, HEAD_DIM), bf16),
            pltpu.VMEM((1, block_len), bf16),
            pltpu.VMEM((2 * blocks, block_len, HEAD_DIM), bf16),
            pltpu.VMEM((2 * blocks, block_len, HEAD_DIM), bf16),
            pltpu.VMEM((blocks, per, 1, tokens), jnp.int32),
            pltpu.VMEM((blocks, 1, block_len), f32),
            pltpu.VMEM((blocks, block_len, LANES), bf16),
            pltpu.VMEM((2, block_len, block_len), bf16),
            pltpu.VMEM((2 * blocks, PARTS, dp, part, HEAD_DIM), bf16),
            pltpu.VMEM((2, block_len, LANES), f32),
            pltpu.VMEM((1, block_len + HEAD_DIM), f32),
            pltpu.VMEM((1, block_len + HEAD_DIM), f32),
            dma((4,)), dma((sp,)), dma((sp,)), dma((sp,)), dma((sp,)),
            dma((sp * PARTS,)), dma((sp * PARTS,)),
            dma((2 * dp * PARTS,)), dma((2 * planes * PARTS,)), dma((2 * PARTS,)),
            dma((2 * planes * PARTS,)), dma, dma((PARTS,)), dma, dma,
            pltpu.SemaphoreType.REGULAR, dma((2 * PARTS,)),
        ],
        compiler_params=pltpu.CompilerParams(
            collective_id=0, has_side_effects=True, vmem_limit_bytes=48 * 1024 * 1024
        ),
    )(
        *[pltpu.with_memory_space_constraint(array, pltpu.HBM) for array in (
            value_in.reshape(tokens, width),
            segments,
            value_gain.reshape(1, HEAD_DIM),
            mixing.reshape(rows, block_len),
            mixing_bias,
        )]
    )
    gated = gelu(gate_in.astype(f32)) * mixed.reshape(sequences, tokens, width).astype(f32)
    return gated.astype(bf16)


def solution(mesh):
    return jax.shard_map(
        per_device,
        mesh=mesh,
        in_specs=(
            P("dp", "sp", None),
            P("dp", "sp", None),
            P("dp", "sp"),
            P("sp"),
            P("sp", "dp", None),
            P("sp", None),
        ),
        out_specs=P("dp", "sp", None),
        check_vma=False,
    )
```

```python
import functools

import jax
import jax.numpy as jnp
from jax import lax
from jax.experimental import pallas as pl
from jax.experimental.pallas import tpu as pltpu
from jax.sharding import PartitionSpec as P

HEAD_DIM = 128
CORES = 2
LANES = 128
ROW_STEP = 256
UNITS = 8
NEAR_PARTS = 4
FAR_SPLIT = ((0, 2), (2, 2), (4, 2), (6, 2))
PARTS = len(FAR_SPLIT)
AHEAD = 2
LAG = 1
MESH = pl.DeviceIdType.MESH

epsilon = 1e-06


def flip(a, b, count):
    total, bit = 0, 1
    while bit < count:
        total = total + ((a // bit + b // bit) % 2) * bit
        bit *= 2
    return total


def gelu(x):
    return jax.nn.gelu(x, approximate=True)


def to_column(row):
    parts = []
    for at in range(0, row.shape[1], LANES):
        piece = jnp.broadcast_to(row[:, at : at + LANES], (LANES, LANES))
        parts.append(piece.T)
    return jnp.concatenate(parts, axis=0)


def kernel(
    sp, dp, value_hbm, ids_hbm, gain_hbm, mixing_ref, bias_hbm, gate_hbm, mixed_ref, act_hbm,
    value_ref, ids_ref, gain_ref, bias_ref, gate_ref,
    act_gate, vals, normed, ids, ids_row, ids_col, mix, res, bias_col, extras, extras_in,
    in_sem, v_send, v_recv, i_send, i_recv, r_send, r_recv,
    mix_recv, across_send, core_send, fwd_send, own_sem, far_send, e_send, e_recv, far_ok, keep_sem, act_sem,
):
    s, d = lax.axis_index("sp"), lax.axis_index("dp")
    tokens = value_ref.shape[0]
    block_len = mix.shape[1]
    per = block_len // tokens
    near = sp // 2
    blocks = near // per
    rows = mixing_ref.shape[0]
    unit = rows // UNITS
    planes = dp // CORES
    half = s % per
    partner = d + 1 - 2 * (d % CORES)
    plane, core = d // CORES, d % CORES
    each = dp // per
    far = flip(s, sp - per, sp)
    level, levels = s // per, sp // per
    mid = (level == levels // 2 - 1) | (level == levels // 2)
    outer = (level < levels // 2 - 1) | (level > levels // 2)

    def across(step):
        return ((plane + step) % planes) * CORES + core

    barrier = pltpu.get_barrier_semaphore()
    for k in range(1, near):
        pl.semaphore_signal(barrier, inc=1, device_id={"sp": flip(s, k, sp)}, device_id_type=MESH)
    pl.semaphore_signal(barrier, inc=1, device_id={"dp": partner}, device_id_type=MESH)
    for step in range(1, planes):
        pl.semaphore_signal(barrier, inc=1, device_id={"dp": across(step)}, device_id_type=MESH)

    @pl.when(mid)
    def _():
        pl.semaphore_signal(barrier, inc=1, device_id={"sp": far}, device_id_type=MESH)

    loads = [
        pltpu.make_async_copy(src, dst, in_sem.at[n])
        for n, (src, dst) in enumerate([
            (value_hbm, value_ref), (ids_hbm, ids_ref), (gain_hbm, gain_ref),
            (bias_hbm, bias_ref), (gate_hbm, gate_ref),
        ])
    ]
    for load in loads:
        load.start()

    count = (1, PARTS)

    def span(which, q):
        if which:
            return FAR_SPLIT[q]
        return q * (UNITS // NEAR_PARTS), UNITS // NEAR_PARTS

    def rows_of(which, origin, q):
        first, units = span(which, q)
        return pl.ds(pl.multiple_of(origin * rows + first * unit, unit), units * unit)

    def chunk(which, origin, q):
        if which:
            return mix.at[1, rows_of(1, origin, q)]
        return mix.at[0, pl.ds(pl.multiple_of(origin * rows, rows), rows)]

    def part_copy(which, src, origin, q, where, sem):
        return pltpu.make_async_remote_copy(
            src_ref=src, dst_ref=chunk(which, origin, q), send_sem=sem,
            recv_sem=mix_recv.at[(which * dp + origin) * PARTS + q],
            device_id=where, device_id_type=MESH,
        )

    def held(which, q):
        return chunk(1, d, q) if which else mixing_ref

    def from_far(q):
        return part_copy(1, mixing_ref.at[rows_of(1, 0, q)], d, q, {"sp": far}, far_send.at[q])

    def to_plane(which, step, q):
        sem = across_send.at[(which * planes + step) * PARTS + q]
        return part_copy(which, held(which, q), d, q, {"dp": across(step)}, sem)

    def to_core(which, q):
        return part_copy(which, held(which, q), d, q, {"dp": partner}, core_send.at[which * PARTS + q])

    def pass_on(which, step, q):
        origin = across(planes - step)
        sem = fwd_send.at[(which * planes + step) * PARTS + q]
        return part_copy(which, chunk(which, origin, q), origin, q, {"dp": partner}, sem)

    def share(which, q):
        for step in range(1, planes):
            to_plane(which, step, q).start()
        to_core(which, q).start()

    def forward(which, q):
        for step in range(1, planes):
            pass_on(which, step, q).wait_recv()
            pass_on(which, step, q).start()

    def arrived(which, q):
        part_copy(which, held(which, q), partner, q, {"dp": partner}, core_send.at[0]).wait_recv()
        for step in range(1, planes):
            origin = across(planes - step)
            there = origin + 1 - 2 * (origin % CORES)
            part_copy(which, held(which, q), there, q, {"dp": partner}, core_send.at[0]).wait_recv()

    def extras_copy():
        return pltpu.make_async_remote_copy(
            src_ref=extras, dst_ref=extras_in, send_sem=e_send, recv_sem=e_recv,
            device_id={"sp": far}, device_id_type=MESH,
        )

    def head_of(owner, which):
        return flip(owner, which * (sp - per), sp)

    def lanes_of(head):
        return pl.ds(pl.multiple_of(head * HEAD_DIM, HEAD_DIM), HEAD_DIM)

    def value_copy(which, k, end):
        target = flip(s, k, sp)
        return pltpu.make_async_remote_copy(
            src_ref=value_ref.at[:, lanes_of(head_of(target, which))],
            dst_ref=vals.at[which * blocks + k // per, pl.ds(pl.multiple_of(end * tokens, tokens), tokens)],
            send_sem=v_send.at[which * near + k], recv_sem=v_recv.at[which * near + k],
            device_id={"sp": target}, device_id_type=MESH,
        )

    def id_copy(k, end):
        return pltpu.make_async_remote_copy(
            src_ref=ids_ref, dst_ref=ids.at[k // per, end],
            send_sem=i_send.at[k], recv_sem=i_recv.at[k],
            device_id={"sp": flip(s, k, sp)}, device_id_type=MESH,
        )

    def place(owner, which, q):
        return mixed_ref.at[:, pl.ds(*span(which, q)), :, lanes_of(head_of(owner, which))]

    def slab(which, block, end, q):
        return res.at[which * blocks + block, pl.ds(end * each, each), pl.ds(*span(which, q))]

    def keep_copy(which, q):
        return pltpu.make_async_copy(
            slab(which, 0, half, q),
            place(s, which, q), keep_sem.at[which * PARTS + q],
        )

    def result_copy(which, k, q):
        target = flip(s, k, sp)
        at = (which * near + k) * PARTS + q
        return pltpu.make_async_remote_copy(
            src_ref=slab(which, k // per, target % per, q),
            dst_ref=place(s, which, q),
            send_sem=r_send.at[at], recv_sem=r_recv.at[at],
            device_id={"sp": target}, device_id_type=MESH,
        )

    loads[2].wait()
    loads[3].wait()
    extras[:, :block_len] = bias_ref[...].astype(jnp.float32)
    extras[:, block_len:] = gain_ref[...].astype(jnp.float32)
    pl.semaphore_wait(barrier, near - 1 + planes + mid.astype(jnp.int32))

    @pl.when(mid)
    def _():
        pl.semaphore_signal(far_ok, inc=1, device_id={"sp": far}, device_id_type=MESH)
        extras_copy().start()
        for q in range(PARTS):
            from_far(q).start()

    share(0, 0)
    own = pltpu.make_async_copy(mixing_ref, chunk(0, d, 0), own_sem)
    own.start()
    loads[0].wait()
    loads[1].wait()

    def send_one(k, carry):
        value_copy(0, k, half).start()
        id_copy(k, half).start()
        return carry

    def send_more(k, carry):
        value_copy(1, k, half).start()
        return carry

    lax.fori_loop(1, near, send_one, 0)
    lax.fori_loop(1, near, send_more, 0)
    for which in (0, 1):
        vals[which * blocks, pl.ds(pl.multiple_of(half * tokens, tokens), tokens), :] = value_ref[:, lanes_of(head_of(s, which))]
    ids[0, half] = ids_ref[...]
    bias_col[0] = to_column(extras[:, :block_len])

    @pl.when(mid)
    def _():
        pl.semaphore_wait(far_ok, 1)
        for k in range(per, near, per):
            pl.semaphore_signal(far_ok, inc=1, device_id={"sp": flip(s, k, sp)}, device_id_type=MESH)

    @pl.when(outer)
    def _():
        pl.semaphore_wait(far_ok, 1)
        extras_copy().start()
        for q in range(PARTS):
            from_far(q).start()

    def norm_block(which, j):
        gain = (extras, extras_in)[which][:, block_len:]
        for i in range(per):
            k = j * per + i

            @pl.when(k > 0)
            def _():
                source_half = flip(s, k, sp) % per
                if which == 0:
                    id_copy(k, source_half).wait_recv()
                value_copy(which, k, source_half).wait_recv()

        n = which * blocks + j
        for at in range(0, block_len, ROW_STEP):
            act = gelu(vals[n, at : at + ROW_STEP, :].astype(jnp.float32))
            mean = jnp.mean(act * act, axis=-1, keepdims=True)
            normed[n, at : at + ROW_STEP, :] = (act * lax.rsqrt(mean + epsilon) * gain).astype(jnp.bfloat16)
        if which == 0:
            row = jnp.concatenate([ids[j, i] for i in range(per)], axis=1).astype(jnp.float32)
            ids_row[j] = row
            ids_col[j] = to_column(row).astype(jnp.bfloat16)

    def norm_blocks(which, first, last):
        def body(j, carry):
            norm_block(which, j)
            return carry

        lax.fori_loop(first, last, body, 0)

    zero = jnp.zeros((), jnp.bfloat16)

    def mix_part(which, q, first=0, last=blocks):
        def body(m, carry):
            j = last - 1 - m
            n = which * blocks + j
            row_b = ids_row[j].astype(jnp.bfloat16)
            right = normed[n]
            tall = []
            for origin in range(dp):
                at = rows_of(which, origin, q)
                col = ids_col[j, at, :]
                wide = []
                for c in range(0, block_len, LANES):
                    same = col == row_b[:, c : c + LANES]
                    piece = mix[which, at, c : c + LANES]
                    wide.append(jnp.where(same, piece, zero))
                tall.append(jnp.concatenate(wide, axis=1))
            summed = jnp.dot(jnp.concatenate(tall, axis=0), right, preferred_element_type=jnp.float32)
            first, units = span(which, q)
            tile = units * unit
            for origin in range(dp):
                bias = bias_col[which, rows_of(which, origin, q), :]
                ready = (summed[origin * tile : (origin + 1) * tile] + bias).astype(jnp.bfloat16)
                res[n, origin, pl.ds(first, units)] = ready.reshape(units, unit, HEAD_DIM)
            for i in range(per):
                k = j * per + i

                @pl.when(k > 0)
                def _():
                    result_copy(which, k, q).start()

                @pl.when(k == 0)
                def _():
                    keep_copy(which, q).start()
            return carry

        lax.fori_loop(0, last - first, body, 0)

    norm_blocks(0, 0, blocks)
    loads[4].wait()

    def gate_rows(n, carry):
        at = pl.ds(pl.multiple_of(n * LANES, LANES), LANES)
        act_gate[at, :] = gelu(gate_ref[at, :].astype(jnp.float32))
        return carry

    lax.fori_loop(0, tokens // LANES, gate_rows, 0)
    act_copy = pltpu.make_async_copy(act_gate, act_hbm, act_sem)
    act_copy.start()

    def relay(q):
        from_far(q).wait_recv()
        share(1, q)

    def near_parts(first, last):
        def body(q, carry):
            mix_part(0, q, first, last)
            return carry

        lax.fori_loop(0, NEAR_PARTS, body, 0)

    def near_here():
        forward(0, 0)
        own.wait()
        arrived(0, 0)
        near_parts(0, blocks)

    def far_values():
        extras_copy().wait_recv()
        bias_col[1] = to_column(extras_in[:, :block_len])
        norm_blocks(1, 0, blocks)

    def far_part(q):
        arrived(1, q)
        mix_part(1, q)

    @pl.when(mid)
    def _():
        for q in range(AHEAD):
            relay(q)
        near_here()
        for q in range(PARTS):
            forward(1, q)
            if q + AHEAD < PARTS:
                relay(q + AHEAD)
            if q == 0:
                far_values()
            else:
                far_part(q - 1)
        far_part(PARTS - 1)

    @pl.when(outer)
    def _():
        near_here()
        for n in range(PARTS + LAG):
            if n < PARTS:
                relay(n)
            if n == LAG:
                far_values()
            if n > LAG:
                far_part(n - LAG - 1)
            if n >= LAG:
                forward(1, n - LAG)
        far_part(PARTS - 1)

    for which in (0, 1):
        for q in range((NEAR_PARTS, PARTS)[which]):
            keep_copy(which, q).wait()

        def collect(k, carry):
            for q in range((NEAR_PARTS, PARTS)[which]):
                result_copy(which, k, q).wait_recv()
            return carry

        lax.fori_loop(1, near, collect, 0)

    def drain(k, carry):
        id_copy(k, half).wait_send()
        for which in (0, 1):
            value_copy(which, k, half).wait_send()
            for q in range((NEAR_PARTS, PARTS)[which]):
                result_copy(which, k, q).wait_send()
        return carry

    lax.fori_loop(1, near, drain, 0)
    act_copy.wait()
    extras_copy().wait_send()
    for q in range(PARTS):
        from_far(q).wait_send()
    for which in (0, 1):
        for q in range(count[which]):
            to_core(which, q).wait_send()
            for step in range(1, planes):
                to_plane(which, step, q).wait_send()
                pass_on(which, step, q).wait_send()


def per_device(gate_in, value_in, segments, value_gain, mixing, mixing_bias):
    sp, dp = lax.axis_size("sp"), lax.axis_size("dp")
    sequences, tokens, width = value_in.shape
    heads_here, rows, block_len = mixing.shape
    assert sequences == 1 and heads_here == 1
    per = block_len // tokens
    near = sp // 2
    blocks = near // per
    planes = dp // CORES
    unit = rows // UNITS
    bf16, f32 = jnp.bfloat16, jnp.float32
    dma = pltpu.SemaphoreType.DMA
    vmem, anywhere = pl.BlockSpec(memory_space=pltpu.VMEM), pl.BlockSpec(memory_space=pl.ANY)
    mixed, act = pl.pallas_call(
        functools.partial(kernel, sp, dp),
        out_shape=(
            jax.ShapeDtypeStruct((dp // per, UNITS, unit, width), bf16),
            jax.ShapeDtypeStruct((tokens, width), f32),
        ),
        in_specs=[anywhere] * 6,
        out_specs=(anywhere, anywhere),
        scratch_shapes=[
            pltpu.VMEM((tokens, width), bf16),
            pltpu.VMEM((1, tokens), jnp.int32),
            pltpu.VMEM((1, HEAD_DIM), bf16),
            pltpu.VMEM((1, block_len), bf16),
            pltpu.VMEM((tokens, width), bf16),
            pltpu.VMEM((tokens, width), f32),
            pltpu.VMEM((2 * blocks, block_len, HEAD_DIM), bf16),
            pltpu.VMEM((2 * blocks, block_len, HEAD_DIM), bf16),
            pltpu.VMEM((blocks, per, 1, tokens), jnp.int32),
            pltpu.VMEM((blocks, 1, block_len), f32),
            pltpu.VMEM((blocks, block_len, LANES), bf16),
            pltpu.VMEM((2, block_len, block_len), bf16),
            pltpu.VMEM((2 * blocks, dp, UNITS, unit, HEAD_DIM), bf16),
            pltpu.VMEM((2, block_len, LANES), f32),
            pltpu.VMEM((1, block_len + HEAD_DIM), f32),
            pltpu.VMEM((1, block_len + HEAD_DIM), f32),
            dma((5,)), dma((sp,)), dma((sp,)), dma((sp,)), dma((sp,)),
            dma((sp * PARTS,)), dma((sp * PARTS,)),
            dma((2 * dp * PARTS,)), dma((2 * planes * PARTS,)), dma((2 * PARTS,)),
            dma((2 * planes * PARTS,)), dma, dma((PARTS,)), dma, dma,
            pltpu.SemaphoreType.REGULAR, dma((2 * PARTS,)), dma,
        ],
        compiler_params=pltpu.CompilerParams(
            collective_id=0, has_side_effects=True, vmem_limit_bytes=44 * 1024 * 1024
        ),
    )(
        *[pltpu.with_memory_space_constraint(array, pltpu.HBM) for array in (
            value_in.reshape(tokens, width),
            segments,
            value_gain.reshape(1, HEAD_DIM),
            mixing.reshape(rows, block_len),
            mixing_bias,
            gate_in.reshape(tokens, width),
        )]
    )
    gated = act * mixed.reshape(tokens, width).astype(f32)
    return gated.astype(bf16).reshape(sequences, tokens, width)


def solution(mesh):
    return jax.shard_map(
        per_device,
        mesh=mesh,
        in_specs=(
            P("dp", "sp", None),
            P("dp", "sp", None),
            P("dp", "sp"),
            P("sp"),
            P("sp", "dp", None),
            P("sp", None),
        ),
        out_specs=P("dp", "sp", None),
        check_vma=False,
    )
```

```python
import functools

import jax
import jax.numpy as jnp
from jax import lax
from jax.experimental import pallas as pl
from jax.experimental.pallas import tpu as pltpu
from jax.sharding import PartitionSpec as P

HEAD_DIM = 128
CORES = 2
LANES = 128
ROW_STEP = 256
UNITS = 8
NEAR_PARTS = 2
FAR_SPLIT = ((0, 2), (2, 2), (4, 2), (6, 2))
PARTS = len(FAR_SPLIT)
AHEAD = 3
LAG = 1
MESH = pl.DeviceIdType.MESH

epsilon = 1e-06


def flip(a, b, count):
    total, bit = 0, 1
    while bit < count:
        total = total + ((a // bit + b // bit) % 2) * bit
        bit *= 2
    return total


def gelu(x):
    return jax.nn.gelu(x, approximate=True)


def to_column(row):
    parts = []
    for at in range(0, row.shape[1], LANES):
        piece = jnp.broadcast_to(row[:, at : at + LANES], (LANES, LANES))
        parts.append(piece.T)
    return jnp.concatenate(parts, axis=0)


def kernel(
    sp, dp, value_hbm, ids_hbm, gain_hbm, mixing_ref, bias_hbm, gate_hbm, mixed_ref, act_hbm,
    value_ref, ids_ref, gain_ref, bias_ref, gate_ref,
    act_gate, vals, normed, ids, ids_row, ids_col, mix, res, bias_col, extras, extras_in,
    in_sem, v_send, v_recv, i_send, i_recv, r_send, r_recv,
    mix_recv, across_send, core_send, fwd_send, own_sem, far_send, e_send, e_recv, far_ok, keep_sem, act_sem,
):
    s, d = lax.axis_index("sp"), lax.axis_index("dp")
    tokens = value_ref.shape[0]
    block_len = mix.shape[1]
    per = block_len // tokens
    near = sp // 2
    blocks = near // per
    rows = mixing_ref.shape[0]
    unit = rows // UNITS
    planes = dp // CORES
    half = s % per
    partner = d + 1 - 2 * (d % CORES)
    plane, core = d // CORES, d % CORES
    each = dp // per
    far = flip(s, sp - per, sp)
    level, levels = s // per, sp // per
    mid = (level == levels // 2 - 1) | (level == levels // 2)
    outer = (level < levels // 2 - 1) | (level > levels // 2)

    def across(step):
        return ((plane + step) % planes) * CORES + core

    barrier = pltpu.get_barrier_semaphore()
    for k in range(1, near):
        pl.semaphore_signal(barrier, inc=1, device_id={"sp": flip(s, k, sp)}, device_id_type=MESH)
    pl.semaphore_signal(barrier, inc=1, device_id={"dp": partner}, device_id_type=MESH)
    for step in range(1, planes):
        pl.semaphore_signal(barrier, inc=1, device_id={"dp": across(step)}, device_id_type=MESH)

    @pl.when(mid)
    def _():
        pl.semaphore_signal(barrier, inc=1, device_id={"sp": far}, device_id_type=MESH)

    loads = [
        pltpu.make_async_copy(src, dst, in_sem.at[n])
        for n, (src, dst) in enumerate([
            (value_hbm, value_ref), (ids_hbm, ids_ref), (gain_hbm, gain_ref),
            (bias_hbm, bias_ref), (gate_hbm, gate_ref),
        ])
    ]
    for load in loads:
        load.start()

    count = (1, PARTS)

    def span(which, q):
        if which:
            return FAR_SPLIT[q]
        return q * (UNITS // NEAR_PARTS), UNITS // NEAR_PARTS

    def rows_of(which, origin, q):
        first, units = span(which, q)
        return pl.ds(pl.multiple_of(origin * rows + first * unit, unit), units * unit)

    def chunk(which, origin, q):
        if which:
            return mix.at[1, rows_of(1, origin, q)]
        return mix.at[0, pl.ds(pl.multiple_of(origin * rows, rows), rows)]

    def part_copy(which, src, origin, q, where, sem):
        return pltpu.make_async_remote_copy(
            src_ref=src, dst_ref=chunk(which, origin, q), send_sem=sem,
            recv_sem=mix_recv.at[(which * dp + origin) * PARTS + q],
            device_id=where, device_id_type=MESH,
        )

    def held(which, q):
        return chunk(1, d, q) if which else mixing_ref

    def from_far(q):
        return part_copy(1, mixing_ref.at[rows_of(1, 0, q)], d, q, {"sp": far}, far_send.at[q])

    def to_plane(which, step, q):
        sem = across_send.at[(which * planes + step) * PARTS + q]
        return part_copy(which, held(which, q), d, q, {"dp": across(step)}, sem)

    def to_core(which, q):
        return part_copy(which, held(which, q), d, q, {"dp": partner}, core_send.at[which * PARTS + q])

    def pass_on(which, step, q):
        origin = across(planes - step)
        sem = fwd_send.at[(which * planes + step) * PARTS + q]
        return part_copy(which, chunk(which, origin, q), origin, q, {"dp": partner}, sem)

    def share(which, q):
        for step in range(1, planes):
            to_plane(which, step, q).start()
        to_core(which, q).start()

    def forward(which, q):
        for step in range(1, planes):
            pass_on(which, step, q).wait_recv()
            pass_on(which, step, q).start()

    def arrived(which, q):
        part_copy(which, held(which, q), partner, q, {"dp": partner}, core_send.at[0]).wait_recv()
        for step in range(1, planes):
            origin = across(planes - step)
            there = origin + 1 - 2 * (origin % CORES)
            part_copy(which, held(which, q), there, q, {"dp": partner}, core_send.at[0]).wait_recv()

    def extras_copy():
        return pltpu.make_async_remote_copy(
            src_ref=extras, dst_ref=extras_in, send_sem=e_send, recv_sem=e_recv,
            device_id={"sp": far}, device_id_type=MESH,
        )

    def head_of(owner, which):
        return flip(owner, which * (sp - per), sp)

    def lanes_of(head):
        return pl.ds(pl.multiple_of(head * HEAD_DIM, HEAD_DIM), HEAD_DIM)

    def value_copy(which, k, end):
        target = flip(s, k, sp)
        return pltpu.make_async_remote_copy(
            src_ref=value_ref.at[:, lanes_of(head_of(target, which))],
            dst_ref=vals.at[which * blocks + k // per, pl.ds(pl.multiple_of(end * tokens, tokens), tokens)],
            send_sem=v_send.at[which * near + k], recv_sem=v_recv.at[which * near + k],
            device_id={"sp": target}, device_id_type=MESH,
        )

    def id_copy(k, end):
        return pltpu.make_async_remote_copy(
            src_ref=ids_ref, dst_ref=ids.at[k // per, end],
            send_sem=i_send.at[k], recv_sem=i_recv.at[k],
            device_id={"sp": flip(s, k, sp)}, device_id_type=MESH,
        )

    def place(owner, which, q):
        return mixed_ref.at[:, pl.ds(*span(which, q)), :, lanes_of(head_of(owner, which))]

    def slab(which, block, end, q):
        return res.at[which * blocks + block, pl.ds(end * each, each), pl.ds(*span(which, q))]

    def keep_copy(which, q):
        return pltpu.make_async_copy(
            slab(which, 0, half, q),
            place(s, which, q), keep_sem.at[which * PARTS + q],
        )

    def result_copy(which, k, q):
        target = flip(s, k, sp)
        at = (which * near + k) * PARTS + q
        return pltpu.make_async_remote_copy(
            src_ref=slab(which, k // per, target % per, q),
            dst_ref=place(s, which, q),
            send_sem=r_send.at[at], recv_sem=r_recv.at[at],
            device_id={"sp": target}, device_id_type=MESH,
        )

    loads[2].wait()
    loads[3].wait()
    extras[:, :block_len] = bias_ref[...].astype(jnp.float32)
    extras[:, block_len:] = gain_ref[...].astype(jnp.float32)
    pl.semaphore_wait(barrier, near - 1 + planes + mid.astype(jnp.int32))

    @pl.when(mid)
    def _():
        pl.semaphore_signal(far_ok, inc=1, device_id={"sp": far}, device_id_type=MESH)
        extras_copy().start()
        for q in range(PARTS):
            from_far(q).start()

    share(0, 0)
    own = pltpu.make_async_copy(mixing_ref, chunk(0, d, 0), own_sem)
    own.start()
    loads[0].wait()
    loads[1].wait()

    def send_one(k, carry):
        value_copy(0, k, half).start()
        id_copy(k, half).start()
        return carry

    def send_more(k, carry):
        value_copy(1, k, half).start()
        return carry

    lax.fori_loop(1, near, send_one, 0)
    lax.fori_loop(1, near, send_more, 0)
    for which in (0, 1):
        vals[which * blocks, pl.ds(pl.multiple_of(half * tokens, tokens), tokens), :] = value_ref[:, lanes_of(head_of(s, which))]
    ids[0, half] = ids_ref[...]
    bias_col[0] = to_column(extras[:, :block_len])

    @pl.when(mid)
    def _():
        pl.semaphore_wait(far_ok, 1)
        for k in range(per, near, per):
            pl.semaphore_signal(far_ok, inc=1, device_id={"sp": flip(s, k, sp)}, device_id_type=MESH)

    @pl.when(outer)
    def _():
        pl.semaphore_wait(far_ok, 1)
        extras_copy().start()
        for q in range(PARTS):
            from_far(q).start()

    def norm_block(which, j):
        gain = (extras, extras_in)[which][:, block_len:]
        for i in range(per):
            k = j * per + i

            @pl.when(k > 0)
            def _():
                source_half = flip(s, k, sp) % per
                if which == 0:
                    id_copy(k, source_half).wait_recv()
                value_copy(which, k, source_half).wait_recv()

        n = which * blocks + j
        for at in range(0, block_len, ROW_STEP):
            act = gelu(vals[n, at : at + ROW_STEP, :].astype(jnp.float32))
            mean = jnp.mean(act * act, axis=-1, keepdims=True)
            normed[n, at : at + ROW_STEP, :] = (act * lax.rsqrt(mean + epsilon) * gain).astype(jnp.bfloat16)
        if which == 0:
            row = jnp.concatenate([ids[j, i] for i in range(per)], axis=1).astype(jnp.float32)
            ids_row[j] = row
            ids_col[j] = to_column(row).astype(jnp.bfloat16)

    def norm_blocks(which, first, last):
        def body(j, carry):
            norm_block(which, j)
            return carry

        lax.fori_loop(first, last, body, 0)

    zero = jnp.zeros((), jnp.bfloat16)

    def mix_part(which, q, first=0, last=blocks, up=False):
        begin = first

        def body(m, carry):
            j = begin + m if up else last - 1 - m
            n = which * blocks + j
            row_b = ids_row[j].astype(jnp.bfloat16)
            right = normed[n]
            tall = []
            for origin in range(dp):
                at = rows_of(which, origin, q)
                col = ids_col[j, at, :]
                wide = []
                for c in range(0, block_len, LANES):
                    same = col == row_b[:, c : c + LANES]
                    piece = mix[which, at, c : c + LANES]
                    wide.append(jnp.where(same, piece, zero))
                tall.append(jnp.concatenate(wide, axis=1))
            summed = jnp.dot(jnp.concatenate(tall, axis=0), right, preferred_element_type=jnp.float32)
            first, units = span(which, q)
            tile = units * unit
            for origin in range(dp):
                bias = bias_col[which, rows_of(which, origin, q), :]
                ready = (summed[origin * tile : (origin + 1) * tile] + bias).astype(jnp.bfloat16)
                res[n, origin, pl.ds(first, units)] = ready.reshape(units, unit, HEAD_DIM)
            for i in range(per):
                k = j * per + i

                @pl.when(k > 0)
                def _():
                    result_copy(which, k, q).start()

                @pl.when(k == 0)
                def _():
                    keep_copy(which, q).start()
            return carry

        lax.fori_loop(0, last - first, body, 0)

    norm_blocks(0, 0, blocks)
    loads[4].wait()

    def gate_rows(n, carry):
        at = pl.ds(pl.multiple_of(n * LANES, LANES), LANES)
        act_gate[at, :] = gelu(gate_ref[at, :].astype(jnp.float32))
        return carry

    lax.fori_loop(0, tokens // LANES, gate_rows, 0)
    act_copy = pltpu.make_async_copy(act_gate, act_hbm, act_sem)
    act_copy.start()

    def relay(q):
        from_far(q).wait_recv()
        share(1, q)

    def near_parts(first, last):
        def body(q, carry):
            mix_part(0, q, first, last)
            return carry

        lax.fori_loop(0, NEAR_PARTS, body, 0)

    def near_here():
        forward(0, 0)
        own.wait()
        arrived(0, 0)
        near_parts(0, blocks)

    def far_values():
        extras_copy().wait_recv()
        bias_col[1] = to_column(extras_in[:, :block_len])
        norm_blocks(1, 0, blocks)

    def far_part(q, up=False):
        arrived(1, q)
        mix_part(1, q, up=up)

    @pl.when(mid)
    def _():
        for q in range(AHEAD):
            relay(q)
        near_here()
        for q in range(PARTS):
            forward(1, q)
            if q + AHEAD < PARTS:
                relay(q + AHEAD)
            if q == 0:
                far_values()
            else:
                far_part(q - 1)
        far_part(PARTS - 1)

    @pl.when(outer)
    def _():
        near_here()
        for n in range(PARTS + LAG):
            if n < PARTS:
                relay(n)
            if n == LAG:
                far_values()
            if n > LAG:
                far_part(n - LAG - 1, True)
            if n >= LAG:
                forward(1, n - LAG)
        far_part(PARTS - 1, True)

    for which in (0, 1):
        for q in range((NEAR_PARTS, PARTS)[which]):
            keep_copy(which, q).wait()

        def collect(k, carry):
            for q in range((NEAR_PARTS, PARTS)[which]):
                result_copy(which, k, q).wait_recv()
            return carry

        lax.fori_loop(1, near, collect, 0)

    def drain(k, carry):
        id_copy(k, half).wait_send()
        for which in (0, 1):
            value_copy(which, k, half).wait_send()
            for q in range((NEAR_PARTS, PARTS)[which]):
                result_copy(which, k, q).wait_send()
        return carry

    lax.fori_loop(1, near, drain, 0)
    act_copy.wait()
    extras_copy().wait_send()
    for q in range(PARTS):
        from_far(q).wait_send()
    for which in (0, 1):
        for q in range(count[which]):
            to_core(which, q).wait_send()
            for step in range(1, planes):
                to_plane(which, step, q).wait_send()
                pass_on(which, step, q).wait_send()


def per_device(gate_in, value_in, segments, value_gain, mixing, mixing_bias):
    sp, dp = lax.axis_size("sp"), lax.axis_size("dp")
    sequences, tokens, width = value_in.shape
    heads_here, rows, block_len = mixing.shape
    assert sequences == 1 and heads_here == 1
    per = block_len // tokens
    near = sp // 2
    blocks = near // per
    planes = dp // CORES
    unit = rows // UNITS
    bf16, f32 = jnp.bfloat16, jnp.float32
    dma = pltpu.SemaphoreType.DMA
    vmem, anywhere = pl.BlockSpec(memory_space=pltpu.VMEM), pl.BlockSpec(memory_space=pl.ANY)
    mixed, act = pl.pallas_call(
        functools.partial(kernel, sp, dp),
        out_shape=(
            jax.ShapeDtypeStruct((dp // per, UNITS, unit, width), bf16),
            jax.ShapeDtypeStruct((tokens, width), f32),
        ),
        in_specs=[anywhere] * 6,
        out_specs=(anywhere, anywhere),
        scratch_shapes=[
            pltpu.VMEM((tokens, width), bf16),
            pltpu.VMEM((1, tokens), jnp.int32),
            pltpu.VMEM((1, HEAD_DIM), bf16),
            pltpu.VMEM((1, block_len), bf16),
            pltpu.VMEM((tokens, width), bf16),
            pltpu.VMEM((tokens, width), f32),
            pltpu.VMEM((2 * blocks, block_len, HEAD_DIM), bf16),
            pltpu.VMEM((2 * blocks, block_len, HEAD_DIM), bf16),
            pltpu.VMEM((blocks, per, 1, tokens), jnp.int32),
            pltpu.VMEM((blocks, 1, block_len), f32),
            pltpu.VMEM((blocks, block_len, LANES), bf16),
            pltpu.VMEM((2, block_len, block_len), bf16),
            pltpu.VMEM((2 * blocks, dp, UNITS, unit, HEAD_DIM), bf16),
            pltpu.VMEM((2, block_len, LANES), f32),
            pltpu.VMEM((1, block_len + HEAD_DIM), f32),
            pltpu.VMEM((1, block_len + HEAD_DIM), f32),
            dma((5,)), dma((sp,)), dma((sp,)), dma((sp,)), dma((sp,)),
            dma((sp * PARTS,)), dma((sp * PARTS,)),
            dma((2 * dp * PARTS,)), dma((2 * planes * PARTS,)), dma((2 * PARTS,)),
            dma((2 * planes * PARTS,)), dma, dma((PARTS,)), dma, dma,
            pltpu.SemaphoreType.REGULAR, dma((2 * PARTS,)), dma,
        ],
        compiler_params=pltpu.CompilerParams(
            collective_id=0, has_side_effects=True, vmem_limit_bytes=44 * 1024 * 1024
        ),
    )(
        *[pltpu.with_memory_space_constraint(array, pltpu.HBM) for array in (
            value_in.reshape(tokens, width),
            segments,
            value_gain.reshape(1, HEAD_DIM),
            mixing.reshape(rows, block_len),
            mixing_bias,
            gate_in.reshape(tokens, width),
        )]
    )
    gated = act * mixed.reshape(tokens, width).astype(f32)
    return gated.astype(bf16).reshape(sequences, tokens, width)


def solution(mesh):
    return jax.shard_map(
        per_device,
        mesh=mesh,
        in_specs=(
            P("dp", "sp", None),
            P("dp", "sp", None),
            P("dp", "sp"),
            P("sp"),
            P("sp", "dp", None),
            P("sp", None),
        ),
        out_specs=P("dp", "sp", None),
        check_vma=False,
    )
```
